32 devices in a mesh: fs: 8 (over z, core), tp: 4 (over y, x).
Axes of the slice: x: 2, y: 2, z: 4, core: 2. Of those that a mesh axis runs over, the one named last changes fastest.
Arguments:
- prompt: bfloat16 [1024, 2048], P('tp'), may hold values from -6 to 6
- norm_gain: float32 [2048], P('fs'), may hold values from 0.1 to 1.9
- gate_master: float32 [32, 2048, 512], P(None, 'fs', 'tp'), may hold values from -6 to 6
- up_master: float32 [32, 2048, 512], P(None, 'fs', 'tp'), may hold values from -6 to 6
- down_master: float32 [32, 2048, 512], P(None, 'fs', 'tp'), may hold values from -6 to 6
- group_choice: int32 [1024], P('tp'), may hold values from 0 to 3
- inner_choice: int32 [1024, 2], P('tp'), may hold values from 0 to 7, as said below
- route_weight: float32 [1024, 2], P('tp'), may hold values from 0.2 to 1
Outputs:
- gate_served: bfloat16 [2048, 16384], P(None, 'fs')
- up_served: bfloat16 [2048, 16384], P(None, 'fs')
- down_served: bfloat16 [2048, 16384], P(None, 'fs')
- mixed: bfloat16 [1024, 2048], P('tp', 'fs')
The draws below stay inside these ranges and needn't reach their ends.
Inputs may be any that keep to these rules, and one draw needn't show every extreme that they name: `inner_choice`: the two experts of a token differ.
All inputs are finite; a program needn't handle non-finite values.
Results may differ from the reference program's by a relative error of at most 0.0081.
Values may be sent and summed in bfloat16 or wider, within the bound.
A program may use at most 128 MiB of HBM per device.

```python
import math
import jax
import jax.numpy as jnp
from jax import lax

D = 2048
FF = 512
GROUPS = 4
EPG = 8
TOK_DEV = 256
EXPERTS = 32
TOKENS = 1024


def routing_draw(key):
    base = jax.random.fold_in(key, 7411)
    keys = jax.random.split(base, 9)
    shards = TOKENS // TOK_DEV
    hot_group = jax.random.randint(keys[0], (shards,), 0, GROUPS)
    hot_inner = jax.random.randint(keys[1], (shards,), 0, EPG)
    hot_count = jax.random.randint(keys[2], (shards,), 0, TOK_DEV // 2 + 1)
    heavy = jax.random.randint(keys[3], (), 0, shards)
    hot_count = jnp.where(jnp.arange(shards) == heavy, 3 * TOK_DEV // 4, hot_count)
    ranks = jax.vmap(lambda sub: jax.random.permutation(sub, TOK_DEV))(jax.random.split(keys[4], shards))
    hot = (ranks < hot_count[:, None]).reshape(TOKENS)
    shard_of = jnp.arange(TOKENS) // TOK_DEV
    drawn_group = jax.random.randint(keys[5], (TOKENS,), 0, GROUPS)
    first_drawn = jax.random.randint(keys[6], (TOKENS,), 0, EPG)
    offsets = jax.random.randint(keys[7], (TOKENS,), 1, EPG)
    flip = jax.random.randint(keys[8], (TOKENS,), 0, 2)
    group = jnp.where(hot, hot_group[shard_of], drawn_group)
    first = jnp.where(hot, hot_inner[shard_of], first_drawn)
    second = (first + offsets) % EPG
    pair = jnp.where(flip[:, None] == 1, jnp.stack([second, first], axis=1), jnp.stack([first, second], axis=1))
    return (group.astype(jnp.int32), pair.astype(jnp.int32))


def draw_group_choice(key, part):
    group, pair = routing_draw(key)
    return group


def draw_inner_choice(key, part):
    group, pair = routing_draw(key)
    return pair


def levels(key, shape, cuts, smallest, high):
    def one(dim, blocks):
        steps = jax.random.uniform(jax.random.fold_in(jax.random.fold_in(key, 6), dim), (blocks,), jnp.float32, smallest / len(cuts), high / len(cuts))
        return jnp.repeat(jnp.exp(steps), shape[dim] // blocks).reshape((-1,) + (1,) * (len(shape) - dim - 1))

    loudness = one(*cuts[0])
    for cut in cuts[1:]:
        loudness = loudness * one(*cut)
    return loudness


def scatter_about(rng, extent, scale, reach, pieces=(), kind=jnp.bfloat16):
    drawn = jax.random.normal(rng, extent, jnp.float32) * scale
    if len(pieces) > 0:
        drawn = levels(rng, extent, pieces, -0.22, 0.18) * drawn
    return jnp.clip(drawn, min=-reach, max=reach).astype(kind)


def setup_inputs(seed: int = 0) -> dict:
    seeds = jax.random.split(jax.random.key(seed), 9)
    prompt = scatter_about(seeds[0], (TOKENS, D), 1.0, 6.0, ((0, 4),))
    norm_gain = jnp.clip(1.0 + 0.18 * jax.random.normal(seeds[1], (D,), jnp.float32), 0.1, 1.9)
    gate_master = scatter_about(seeds[2], (EXPERTS, D, FF), 1.0, 6.0, ((1, 8), (2, 4)), jnp.float32)
    up_master = scatter_about(seeds[3], (EXPERTS, D, FF), 1.0, 6.0, ((1, 8), (2, 4)), jnp.float32)
    down_master = scatter_about(seeds[4], (EXPERTS, D, FF), 1.0, 6.0, ((1, 8), (2, 4)), jnp.float32)
    group_choice = draw_group_choice(jax.random.fold_in(seeds[8], 71), 0)
    inner_choice = draw_inner_choice(jax.random.fold_in(seeds[8], 71), 0)
    route_weight = jnp.clip(jnp.exp(math.log(1.0) - 1.609438 * jax.random.uniform(seeds[7], (TOKENS, 2), jnp.float32) ** levels(seeds[7], (TOKENS, 2), ((0, 4),), -0.2, 0.2)), 0.2, 1.0)
    return dict(prompt=prompt, norm_gain=norm_gain, gate_master=gate_master, up_master=up_master, down_master=down_master, group_choice=group_choice, inner_choice=inner_choice, route_weight=route_weight)


def reference(prompt, norm_gain, gate_master, up_master, down_master, group_choice, inner_choice, route_weight):
    experts = GROUPS * EPG
    scale = norm_gain[None, :, None]
    gate_served = (gate_master * scale).astype(jnp.bfloat16).transpose(1, 0, 2).reshape(D, experts * FF)
    up_served = (up_master * scale).astype(jnp.bfloat16).transpose(1, 0, 2).reshape(D, experts * FF)
    down_served = down_master.astype(jnp.bfloat16).transpose(1, 0, 2).reshape(D, experts * FF)
    values = prompt.astype(jnp.float32)
    normed = (values * lax.rsqrt(lax.optimization_barrier(jnp.mean(values * values, axis=1, keepdims=True)) + 1e-06)).astype(jnp.bfloat16)
    chosen = group_choice[:, None] * EPG + inner_choice
    member = (chosen[:, :, None] == jnp.arange(experts, dtype=jnp.int32)[None, None, :]).astype(jnp.float32)
    weight = lax.optimization_barrier(jnp.sum(member * route_weight[:, :, None], axis=1))

    def one_expert(total, index):
        begin = (index * FF).astype(jnp.int32)
        gate_cols = lax.dynamic_slice_in_dim(gate_served, begin, FF, 1)
        up_cols = lax.dynamic_slice_in_dim(up_served, begin, FF, 1)
        down_cols = lax.dynamic_slice_in_dim(down_served, begin, FF, 1)
        gate_act = jnp.dot(normed, gate_cols, preferred_element_type=jnp.float32) * D ** (-0.5)
        up_act = jnp.dot(normed, up_cols, preferred_element_type=jnp.float32) * D ** (-0.5)
        column = lax.dynamic_slice_in_dim(weight, index.astype(jnp.int32), 1, 1)
        scaled = (column * jax.nn.silu(gate_act) * up_act).astype(jnp.bfloat16)
        part = lax.dot_general(scaled, down_cols, (((1,), (1,)), ((), ())), preferred_element_type=jnp.float32)
        return (total + part, None)
    total, _ = lax.scan(one_expert, jnp.zeros((prompt.shape[0], D), jnp.float32), jnp.arange(experts, dtype=jnp.int32))
    mixed = (total * FF ** (-0.5)).astype(jnp.bfloat16)
    return (gate_served, up_served, down_served, mixed)
```

```python
import functools

import jax
import jax.numpy as jnp
from jax import lax
from jax.experimental import pallas as pl
from jax.experimental.pallas import tpu as pltpu
from jax.sharding import PartitionSpec as P

MESH = pl.DeviceIdType.MESH
FF = 512
GROUPS = 4
EPG = 8


def flatten_rows(piece):
    count, experts, rows, hidden = piece.shape
    return piece.transpose(0, 2, 1, 3).reshape(count, rows, experts * hidden)


def restore_rows(gathered, rows):
    parts = lax.axis_size("tp")
    count, total, width = gathered.shape
    blocks = total // (parts * rows)
    ordered = gathered.reshape(count, parts, blocks, rows, width).transpose(0, 2, 1, 3, 4)
    return ordered.reshape(count, total, width)


def activations(normed, gate_local, up_local, column_weight):
    width = normed.shape[1]
    gate_act = jnp.dot(normed, gate_local, preferred_element_type=jnp.float32) * width ** (-0.5)
    up_act = jnp.dot(normed, up_local, preferred_element_type=jnp.float32) * width ** (-0.5)
    return (column_weight * jax.nn.silu(gate_act) * up_act).astype(jnp.bfloat16)


def route_columns(weight, columns, experts):
    first = lax.axis_index("fs") * columns
    owner = (first + jnp.arange(columns, dtype=jnp.int32)) // FF
    onehot = (owner[None, :] == jnp.arange(experts, dtype=jnp.int32)[:, None]).astype(jnp.float32)
    return jnp.dot(weight, onehot, precision=lax.Precision.HIGHEST)


def shards(
    prompt, norm_gain, gate_master, up_master, down_master, group_choice, inner_choice, route_weight
):
    experts = GROUPS * EPG
    scale = norm_gain[None, :, None]
    gate_cast = (gate_master * scale).astype(jnp.bfloat16)
    up_cast = (up_master * scale).astype(jnp.bfloat16)
    down_cast = down_master.astype(jnp.bfloat16)
    rows = gate_master.shape[1] // lax.axis_size("tp")
    values = prompt.astype(jnp.float32)
    normed = (values * lax.rsqrt(jnp.mean(values * values, axis=1, keepdims=True) + 1e-06)).astype(
        jnp.bfloat16
    )
    chosen = group_choice[:, None] * EPG + inner_choice
    member = (chosen[:, :, None] == jnp.arange(experts, dtype=jnp.int32)[None, None, :]).astype(
        jnp.float32
    )
    weight = jnp.sum(member * route_weight[:, :, None], axis=1)
    stacked = jnp.stack([gate_cast, up_cast, down_cast])
    widened = lax.all_to_all(stacked, "tp", split_axis=2, concat_axis=3, tiled=True)
    moved = lax.all_to_all(flatten_rows(widened), "fs", split_axis=2, concat_axis=1, tiled=True)
    served = restore_rows(lax.all_gather(moved, "tp", axis=1, tiled=True), rows)
    gate_local, up_local, down_local = (served[0], served[1], served[2])
    column_weight = route_columns(weight, gate_local.shape[1], experts)
    scaled = activations(normed, gate_local, up_local, column_weight)
    summed = lax.psum_scatter(
        lax.dot_general(
            down_local, scaled, (((1,), (1,)), ((), ())), preferred_element_type=jnp.float32
        ),
        "fs",
        scatter_dimension=0,
        tiled=True,
    )
    mixed = (summed * FF ** (-0.5)).T.astype(jnp.bfloat16)
    return (gate_local, up_local, down_local, mixed)


def cast_body(scale_ref, gate_ref, up_ref, down_ref, out_ref):
    scale = scale_ref[...][None]
    out_ref[0, 0] = (gate_ref[0] * scale).astype(jnp.bfloat16)
    out_ref[1, 0] = (up_ref[0] * scale).astype(jnp.bfloat16)
    out_ref[2, 0] = down_ref[0].astype(jnp.bfloat16)


def cast_masters(norm_gain, gate_master, up_master, down_master, groups):
    experts, rows, hidden = gate_master.shape
    per = experts // groups
    views = [part.reshape(groups, per, rows, hidden) for part in (gate_master, up_master, down_master)]
    scale = jnp.broadcast_to(norm_gain[:, None], (rows, hidden))
    block = pl.BlockSpec((1, per, rows, hidden), lambda i: (i, 0, 0, 0))
    return pl.pallas_call(
        cast_body,
        grid=(groups,),
        in_specs=[pl.BlockSpec((rows, hidden), lambda i: (0, 0)), block, block, block],
        out_specs=pl.BlockSpec((3, 1, per, rows, hidden), lambda i: (0, i, 0, 0, 0)),
        out_shape=jax.ShapeDtypeStruct((3, groups, per, rows, hidden), jnp.bfloat16),
        name="cast",
    )(scale, *views)


def spread_body(groups, cast_ref, staged_ref, own, own_in, own_out, zs, zr, xs, xr, ys, yr, fxs, fxr, fys, fyr):
    f, t = lax.axis_index("fs"), lax.axis_index("tp")
    tx, ty, td = jnp.bitwise_xor(t, 1), jnp.bitwise_xor(t, 2), jnp.bitwise_xor(t, 3)
    half = cast_ref.shape[2] // 2

    def peer(k):
        return jnp.bitwise_xor(f, k)

    def z_copy(w, k):
        return pltpu.make_async_remote_copy(
            src_ref=cast_ref.at[w, peer(k)],
            dst_ref=staged_ref.at[w, t, f],
            send_sem=zs.at[w, k],
            recv_sem=zr.at[w, k],
            device_id={"fs": peer(k), "tp": t},
            device_id_type=MESH,
        )

    def z_arrival(w, k):
        return pltpu.make_async_remote_copy(
            src_ref=cast_ref.at[w, peer(k)],
            dst_ref=staged_ref.at[w, t, peer(k)],
            send_sem=zs.at[w, k],
            recv_sem=zr.at[w, k],
            device_id={"fs": peer(k), "tp": t},
            device_id_type=MESH,
        )

    def side_copy(w, k, origin, target, send, recv):
        block = staged_ref.at[w, origin, peer(k)]
        source = cast_ref.at[w, f] if k == 0 and origin is t else block
        return pltpu.make_async_remote_copy(
            src_ref=source,
            dst_ref=block,
            send_sem=send.at[w, k],
            recv_sem=recv.at[w, k],
            device_id={"fs": f, "tp": target},
            device_id_type=MESH,
        )

    def half_copy(w, k, origin, part, target, send, recv):
        block = staged_ref.at[w, origin, peer(k), pl.ds(part * half, half)]
        return pltpu.make_async_remote_copy(
            src_ref=block,
            dst_ref=block,
            send_sem=send.at[w, k],
            recv_sem=recv.at[w, k],
            device_id={"fs": f, "tp": target},
            device_id_type=MESH,
        )

    def forward(w, k):
        side_copy(w, k, tx, tx, xs, xr).wait_recv()
        half_copy(w, k, tx, 0, ty, fys, fyr).start()
        side_copy(w, k, ty, ty, ys, yr).wait_recv()
        half_copy(w, k, ty, 1, tx, fxs, fxr).start()

    barrier = pltpu.get_barrier_semaphore()
    for k in range(1, groups):
        pl.semaphore_signal(barrier, inc=1, device_id={"fs": peer(k), "tp": t}, device_id_type=MESH)
    for other in (tx, ty):
        pl.semaphore_signal(barrier, inc=1, device_id={"fs": f, "tp": other}, device_id_type=MESH)
    pl.semaphore_wait(barrier, groups + 1)

    for k in range(1, groups):
        z_copy(0, k).start()

    def one_array(w, carry):
        for k in range(groups):
            if k > 0:
                z_arrival(w, k).wait_recv()
            side_copy(w, k, t, tx, xs, xr).start()
            side_copy(w, k, t, ty, ys, yr).start()
            if k > 0:

                @pl.when(w < 2)
                def _():
                    z_copy(w + 1, k).start()

                forward(w, k - 1)
            else:

                @pl.when(w > 0)
                def _():
                    forward(w - 1, groups - 1)

                pltpu.make_async_copy(cast_ref.at[w, f], own.at[w], own_in.at[w]).start()
            if k == 1:
                pltpu.make_async_copy(cast_ref.at[w, f], own.at[w], own_in.at[w]).wait()
                pltpu.make_async_copy(own.at[w], staged_ref.at[w, t, f], own_out.at[w]).start()
        return carry

    lax.fori_loop(0, 3, one_array, 0)
    forward(2, groups - 1)

    def finish(w, carry):
        pltpu.make_async_copy(own.at[w], staged_ref.at[w, t, f], own_out.at[w]).wait()
        for k in range(groups):
            if k > 0:
                z_copy(w, k).wait_send()
            side_copy(w, k, t, tx, xs, xr).wait_send()
            side_copy(w, k, t, ty, ys, yr).wait_send()
            half_copy(w, k, tx, 0, ty, fys, fyr).wait_send()
            half_copy(w, k, ty, 1, tx, fxs, fxr).wait_send()
            half_copy(w, k, td, 0, ty, fys, fyr).wait_recv()
            half_copy(w, k, td, 1, tx, fxs, fxr).wait_recv()
        return carry

    lax.fori_loop(0, 3, finish, 0)


def spread(cast, parts):
    arrays, groups, per, rows, hidden = cast.shape
    return pl.pallas_call(
        functools.partial(spread_body, groups),
        in_specs=[pl.BlockSpec(memory_space=pl.ANY)],
        out_specs=pl.BlockSpec(memory_space=pl.ANY),
        out_shape=jax.ShapeDtypeStruct((arrays, parts, groups, per, rows, hidden), cast.dtype),
        scratch_shapes=[
            pltpu.VMEM((arrays, per, rows, hidden), cast.dtype),
            pltpu.SemaphoreType.DMA((arrays,)),
            pltpu.SemaphoreType.DMA((arrays,)),
        ]
        + [pltpu.SemaphoreType.DMA((arrays, groups))] * 10,
        compiler_params=pltpu.CompilerParams(collective_id=0, has_side_effects=True),
        name="spread",
    )(cast)


def serve_body(normed_ref, weight_ref, staged_ref, gate_ref, up_ref, down_ref, part_ref):
    _, parts, groups, _, rows, hidden = staged_ref.shape
    for w, out in enumerate((gate_ref, up_ref, down_ref)):
        for t in range(parts):
            out[:, t * hidden : (t + 1) * hidden] = staged_ref[w, t, :, 0].reshape(groups * rows, hidden)
    normed = normed_ref[...]
    scaled = activations(normed, gate_ref[...], up_ref[...], weight_ref[0])
    part = lax.dot_general(
        scaled, down_ref[...], (((1,), (1,)), ((), ())), preferred_element_type=jnp.float32
    )

    @pl.when(pl.program_id(0) == 0)
    def _():
        part_ref[...] = part

    @pl.when(pl.program_id(0) > 0)
    def _():
        part_ref[...] += part


def serve(normed, weight, staged):
    arrays, parts, groups, per, rows, hidden = staged.shape
    tokens, width = normed.shape
    out = jax.ShapeDtypeStruct((width, per * parts * hidden), staged.dtype)
    block = pl.BlockSpec((width, parts * hidden), lambda e: (0, e))
    return pl.pallas_call(
        serve_body,
        grid=(per,),
        in_specs=[
            pl.BlockSpec((tokens, width), lambda e: (0, 0)),
            pl.BlockSpec((1, tokens, 1), lambda e: (e, 0, 0)),
            pl.BlockSpec((arrays, parts, groups, 1, rows, hidden), lambda e: (0, 0, 0, e, 0, 0)),
        ],
        out_specs=[block, block, block, pl.BlockSpec((tokens, width), lambda e: (0, 0))],
        out_shape=[out, out, out, jax.ShapeDtypeStruct((tokens, width), jnp.float32)],
        compiler_params=pltpu.CompilerParams(vmem_limit_bytes=60 * 1024 * 1024),
        name="serve",
    )(normed, weight, staged)


def direct_shards(
    prompt, norm_gain, gate_master, up_master, down_master, group_choice, inner_choice, route_weight
):
    groups, parts = lax.axis_size("fs"), lax.axis_size("tp")
    per = gate_master.shape[0] // groups
    staged = spread(cast_masters(norm_gain, gate_master, up_master, down_master, groups), parts)
    values = prompt.astype(jnp.float32)
    normed = (values * lax.rsqrt(jnp.mean(values * values, axis=1, keepdims=True) + 1e-06)).astype(
        jnp.bfloat16
    )
    chosen = group_choice[:, None] * EPG + inner_choice
    mine = lax.axis_index("fs") * per + jnp.arange(per, dtype=jnp.int32)
    member = (chosen[None] == mine[:, None, None]).astype(jnp.float32)
    weight = jnp.sum(member * route_weight[None], axis=2)[:, :, None]
    gate_local, up_local, down_local, part = serve(normed, weight, staged)
    summed = lax.psum_scatter(part, "fs", scatter_dimension=1, tiled=True)
    mixed = (summed * FF ** (-0.5)).astype(jnp.bfloat16)
    return (gate_local, up_local, down_local, mixed)


def fits_direct(mesh):
    groups, parts = mesh.shape["fs"], mesh.shape["tp"]
    whole_experts = (GROUPS * EPG) % groups == 0 and (GROUPS * EPG // groups) % 2 == 0
    return parts == 4 and groups & (groups - 1) == 0 and whole_experts and FF // parts % 128 == 0


def solution(mesh):
    in_specs = (
        P("tp", None),
        P("fs"),
        P(None, "fs", "tp"),
        P(None, "fs", "tp"),
        P(None, "fs", "tp"),
        P("tp"),
        P("tp", None),
        P("tp", None),
    )
    out_specs = (P(None, "fs"), P(None, "fs"), P(None, "fs"), P("tp", "fs"))
    body = direct_shards if fits_direct(mesh) else shards
    return jax.shard_map(body, mesh=mesh, in_specs=in_specs, out_specs=out_specs, check_vma=False)
```

```python
import functools

import jax
import jax.numpy as jnp
from jax import lax
from jax.experimental import pallas as pl
from jax.experimental.pallas import tpu as pltpu
from jax.sharding import PartitionSpec as P

MESH = pl.DeviceIdType.MESH
FF = 512
GROUPS = 4
EPG = 8


def flatten_rows(piece):
    count, experts, rows, hidden = piece.shape
    return piece.transpose(0, 2, 1, 3).reshape(count, rows, experts * hidden)


def restore_rows(gathered, rows):
    parts = lax.axis_size("tp")
    count, total, width = gathered.shape
    blocks = total // (parts * rows)
    ordered = gathered.reshape(count, parts, blocks, rows, width).transpose(0, 2, 1, 3, 4)
    return ordered.reshape(count, total, width)


def activations(normed, gate_local, up_local, column_weight):
    width = normed.shape[1]
    gate_act = jnp.dot(normed, gate_local, preferred_element_type=jnp.float32) * width ** (-0.5)
    up_act = jnp.dot(normed, up_local, preferred_element_type=jnp.float32) * width ** (-0.5)
    return (column_weight * jax.nn.silu(gate_act) * up_act).astype(jnp.bfloat16)


def route_columns(weight, columns, experts):
    first = lax.axis_index("fs") * columns
    owner = (first + jnp.arange(columns, dtype=jnp.int32)) // FF
    onehot = (owner[None, :] == jnp.arange(experts, dtype=jnp.int32)[:, None]).astype(jnp.float32)
    return jnp.dot(weight, onehot, precision=lax.Precision.HIGHEST)


def shards(
    prompt, norm_gain, gate_master, up_master, down_master, group_choice, inner_choice, route_weight
):
    experts = GROUPS * EPG
    scale = norm_gain[None, :, None]
    gate_cast = (gate_master * scale).astype(jnp.bfloat16)
    up_cast = (up_master * scale).astype(jnp.bfloat16)
    down_cast = down_master.astype(jnp.bfloat16)
    rows = gate_master.shape[1] // lax.axis_size("tp")
    values = prompt.astype(jnp.float32)
    normed = (values * lax.rsqrt(jnp.mean(values * values, axis=1, keepdims=True) + 1e-06)).astype(
        jnp.bfloat16
    )
    chosen = group_choice[:, None] * EPG + inner_choice
    member = (chosen[:, :, None] == jnp.arange(experts, dtype=jnp.int32)[None, None, :]).astype(
        jnp.float32
    )
    weight = jnp.sum(member * route_weight[:, :, None], axis=1)
    stacked = jnp.stack([gate_cast, up_cast, down_cast])
    widened = lax.all_to_all(stacked, "tp", split_axis=2, concat_axis=3, tiled=True)
    moved = lax.all_to_all(flatten_rows(widened), "fs", split_axis=2, concat_axis=1, tiled=True)
    served = restore_rows(lax.all_gather(moved, "tp", axis=1, tiled=True), rows)
    gate_local, up_local, down_local = (served[0], served[1], served[2])
    column_weight = route_columns(weight, gate_local.shape[1], experts)
    scaled = activations(normed, gate_local, up_local, column_weight)
    summed = lax.psum_scatter(
        lax.dot_general(
            down_local, scaled, (((1,), (1,)), ((), ())), preferred_element_type=jnp.float32
        ),
        "fs",
        scatter_dimension=0,
        tiled=True,
    )
    mixed = (summed * FF ** (-0.5)).T.astype(jnp.bfloat16)
    return (gate_local, up_local, down_local, mixed)


def cast_body(scale_ref, gate_ref, up_ref, down_ref, out_ref):
    hidden = out_ref.shape[-1]
    scale = jnp.broadcast_to(scale_ref[...], (hidden, scale_ref.shape[1])).T[None]
    out_ref[0, 0] = (gate_ref[0] * scale).astype(jnp.bfloat16)
    out_ref[1, 0] = (up_ref[0] * scale).astype(jnp.bfloat16)
    out_ref[2, 0] = down_ref[0].astype(jnp.bfloat16)


def cast_masters(norm_gain, gate_master, up_master, down_master, groups):
    experts, rows, hidden = gate_master.shape
    per = experts // groups
    views = [part.reshape(groups, per, rows, hidden) for part in (gate_master, up_master, down_master)]
    block = pl.BlockSpec((1, per, rows, hidden), lambda i: (i, 0, 0, 0))
    return pl.pallas_call(
        cast_body,
        grid=(groups,),
        in_specs=[pl.BlockSpec((1, rows), lambda i: (0, 0)), block, block, block],
        out_specs=pl.BlockSpec((3, 1, per, rows, hidden), lambda i: (0, i, 0, 0, 0)),
        out_shape=jax.ShapeDtypeStruct((3, groups, per, rows, hidden), jnp.bfloat16),
        name="cast",
    )(norm_gain.reshape(1, rows), *views)


def spread_body(
    groups,
    cast_ref,
    prompt_ref,
    group_ref,
    inner_ref,
    route_ref,
    staged_ref,
    mixed_ref,
    own,
    normed,
    held,
    scaled,
    down,
    part,
    got,
    own_in,
    own_out,
    held_sem,
    down_sem,
    ps,
    pr,
    zs,
    zr,
    xs,
    xr,
    ys,
    yr,
    fxs,
    fxr,
    fys,
    fyr,
):
    f, t = lax.axis_index("fs"), lax.axis_index("tp")
    tx, ty, td = jnp.bitwise_xor(t, 1), jnp.bitwise_xor(t, 2), jnp.bitwise_xor(t, 3)
    half = cast_ref.shape[2] // 2

    def peer(k):
        return jnp.bitwise_xor(f, k)

    def z_copy(w, k):
        return pltpu.make_async_remote_copy(
            src_ref=cast_ref.at[w, peer(k)],
            dst_ref=staged_ref.at[w, t, f],
            send_sem=zs.at[w, k],
            recv_sem=zr.at[w, k],
            device_id={"fs": peer(k), "tp": t},
            device_id_type=MESH,
        )

    def z_arrival(w, k):
        return pltpu.make_async_remote_copy(
            src_ref=cast_ref.at[w, peer(k)],
            dst_ref=staged_ref.at[w, t, peer(k)],
            send_sem=zs.at[w, k],
            recv_sem=zr.at[w, k],
            device_id={"fs": peer(k), "tp": t},
            device_id_type=MESH,
        )

    def side_copy(w, k, origin, target, send, recv):
        block = staged_ref.at[w, origin, peer(k)]
        source = cast_ref.at[w, f] if k == 0 and origin is t else block
        return pltpu.make_async_remote_copy(
            src_ref=source,
            dst_ref=block,
            send_sem=send.at[w, k],
            recv_sem=recv.at[w, k],
            device_id={"fs": f, "tp": target},
            device_id_type=MESH,
        )

    def half_copy(w, k, origin, part, target, send, recv):
        block = staged_ref.at[w, origin, peer(k), pl.ds(part * half, half)]
        return pltpu.make_async_remote_copy(
            src_ref=block,
            dst_ref=block,
            send_sem=send.at[w, k],
            recv_sem=recv.at[w, k],
            device_id={"fs": f, "tp": target},
            device_id_type=MESH,
        )

    def forward(w, k):
        side_copy(w, k, tx, tx, xs, xr).wait_recv()
        half_copy(w, k, tx, 0, ty, fys, fyr).start()
        side_copy(w, k, ty, ty, ys, yr).wait_recv()
        half_copy(w, k, ty, 1, tx, fxs, fxr).start()

    barrier = pltpu.get_barrier_semaphore()
    for k in range(1, groups):
        pl.semaphore_signal(barrier, inc=1, device_id={"fs": peer(k), "tp": t}, device_id_type=MESH)
    for other in (tx, ty):
        pl.semaphore_signal(barrier, inc=1, device_id={"fs": f, "tp": other}, device_id_type=MESH)
    pl.semaphore_wait(barrier, groups + 1)

    for k in range(1, groups):
        z_copy(0, k).start()

    def diagonal_wait(w, k):
        half_copy(w, k, td, 0, ty, fys, fyr).wait_recv()
        half_copy(w, k, td, 1, tx, fxs, fxr).wait_recv()

    def own_load(w):
        return pltpu.make_async_copy(cast_ref.at[w, f], own.at[w], own_in.at[w])

    def own_store(w):
        return pltpu.make_async_copy(own.at[w], staged_ref.at[w, t, f], own_out.at[w])

    def part_copy(k):
        return pltpu.make_async_remote_copy(
            src_ref=part.at[k],
            dst_ref=got.at[k],
            send_sem=ps.at[k],
            recv_sem=pr.at[k],
            device_id={"fs": peer(k), "tp": t},
            device_id_type=MESH,
        )

    parts, _, per, rows, hidden = staged_ref.shape[1:]
    tokens, width = prompt_ref.shape

    def one_array(w, carry):
        for k in range(groups):
            if k > 0:
                z_arrival(w, k).wait_recv()
            side_copy(w, k, t, tx, xs, xr).start()
            side_copy(w, k, t, ty, ys, yr).start()
            if k > 0:
                z_copy(w + 1, k * (1 - w) + (groups - k) * w).start()
                forward(w, k - 1)
            else:

                @pl.when(w > 0)
                def _():
                    forward(w - 1, groups - 1)

                own_load(w).start()
            if k == 1:
                own_load(w).wait()
                own_store(w).start()
        return carry

    def normalise():
        values = prompt_ref[...].astype(jnp.float32)
        mean = jnp.mean(values * values, axis=1, keepdims=True)
        normed[...] = (values * lax.rsqrt(mean + 1e-06)).astype(jnp.bfloat16)

    def hidden_units(e, carry):
        loads = [pltpu.make_async_copy(staged_ref.at[w, :, :, e], held.at[w], held_sem.at[w]) for w in range(2)]
        for load in loads:
            load.start()
        chosen = group_ref[...] * EPG + inner_ref[...]
        weight = jnp.sum(jnp.where(chosen == f * per + e, route_ref[...], 0.0), axis=0, keepdims=True)
        column = jnp.broadcast_to(weight, (hidden, tokens)).T
        for load in loads:
            load.wait()

        def one_part(i, inner):
            gate = held[0, i].reshape(groups * rows, hidden)
            up = held[1, i].reshape(groups * rows, hidden)
            scaled[e, i] = activations(normed[...], gate, up, column)
            return inner

        return lax.fori_loop(0, parts, one_part, carry)

    def features(k):
        diagonal_wait(2, k)
        if k == 0:
            own_store(2).wait()
        load = pltpu.make_async_copy(staged_ref.at[2, :, peer(k)], down, down_sem)
        load.start()
        part[k] = jnp.zeros_like(part[k])
        load.wait()

        def one_expert(e, carry):
            left = jnp.concatenate([scaled[e, i] for i in range(parts)], axis=1)
            right = jnp.concatenate([down[i, e] for i in range(parts)], axis=1)
            part[k] += lax.dot_general(
                left, right, (((1,), (1,)), ((), ())), preferred_element_type=jnp.float32
            )
            return carry

        lax.fori_loop(0, per, one_expert, 0)
        if k > 0:
            part_copy(k).start()

    lax.fori_loop(0, 2, one_array, 0)

    order = list(range(groups - 1, -1, -1))
    done = 0
    for i, k in enumerate(order):
        if k > 0:
            z_arrival(2, k).wait_recv()
        side_copy(2, k, t, tx, xs, xr).start()
        side_copy(2, k, t, ty, ys, yr).start()
        if i == 0:
            own_load(2).start()
            forward(1, groups - 1)
            normalise()
        else:
            forward(2, order[i - 1])
        if i == 1:
            own_load(2).wait()
            own_store(2).start()
            for w in range(2):
                own_store(w).wait()
                for other in range(groups):
                    diagonal_wait(w, other)
            lax.fori_loop(0, per // 2, hidden_units, 0)
        if i == 2:
            lax.fori_loop(per // 2, per, hidden_units, 0)
        while i >= 3 and done <= i - 2:
            features(order[done])
            done += 1
    forward(2, order[-1])
    while done < groups:
        features(order[done])
        done += 1

    total = part[0]
    for k in range(groups - 1, 0, -1):
        part_copy(k).wait_recv()
        total = total + got[k]
    mixed_ref[...] = (total * FF ** (-0.5)).astype(jnp.bfloat16)

    def finish(w, carry):
        for k in range(groups):
            if k > 0:
                z_copy(w, k).wait_send()
            side_copy(w, k, t, tx, xs, xr).wait_send()
            side_copy(w, k, t, ty, ys, yr).wait_send()
            half_copy(w, k, tx, 0, ty, fys, fyr).wait_send()
            half_copy(w, k, ty, 1, tx, fxs, fxr).wait_send()
        return carry

    lax.fori_loop(0, 3, finish, 0)
    for k in range(1, groups):
        part_copy(k).wait_send()


def spread(cast, prompt, group_choice, inner_choice, route_weight, parts):
    arrays, groups, per, rows, hidden = cast.shape
    tokens, width = prompt.shape
    vmem = pl.BlockSpec(memory_space=pltpu.VMEM)
    return pl.pallas_call(
        functools.partial(spread_body, groups),
        in_specs=[pl.BlockSpec(memory_space=pl.ANY), vmem, vmem, vmem, vmem],
        out_specs=[pl.BlockSpec(memory_space=pl.ANY), vmem],
        out_shape=[
            jax.ShapeDtypeStruct((arrays, parts, groups, per, rows, hidden), cast.dtype),
            jax.ShapeDtypeStruct((tokens, width // groups), jnp.bfloat16),
        ],
        scratch_shapes=[
            pltpu.VMEM((arrays, per, rows, hidden), cast.dtype),
            pltpu.VMEM((tokens, width), jnp.bfloat16),
            pltpu.VMEM((2, parts, groups, rows, hidden), cast.dtype),
            pltpu.VMEM((per, parts, tokens, hidden), jnp.bfloat16),
            pltpu.VMEM((parts, per, rows, hidden), cast.dtype),
            pltpu.VMEM((groups, tokens, rows), jnp.float32),
            pltpu.VMEM((groups, tokens, rows), jnp.float32),
            pltpu.SemaphoreType.DMA((arrays,)),
            pltpu.SemaphoreType.DMA((arrays,)),
            pltpu.SemaphoreType.DMA((2,)),
            pltpu.SemaphoreType.DMA,
            pltpu.SemaphoreType.DMA((groups,)),
            pltpu.SemaphoreType.DMA((groups,)),
        ]
        + [pltpu.SemaphoreType.DMA((arrays, groups))] * 10,
        compiler_params=pltpu.CompilerParams(
            collective_id=0, has_side_effects=True, vmem_limit_bytes=60 * 1024 * 1024
        ),
        name="spread",
    )(cast, prompt, group_choice.reshape(1, tokens), inner_choice.T, route_weight.T)


def serve_body(staged_ref, gate_ref, up_ref, down_ref):
    _, parts, groups, _, rows, hidden = staged_ref.shape
    for w, out in enumerate((gate_ref, up_ref, down_ref)):
        for t in range(parts):
            out[:, t * hidden : (t + 1) * hidden] = staged_ref[w, t, :, 0].reshape(groups * rows, hidden)


def serve(staged):
    arrays, parts, groups, per, rows, hidden = staged.shape
    width = groups * rows
    out = jax.ShapeDtypeStruct((width, per * parts * hidden), staged.dtype)
    block = pl.BlockSpec((width, parts * hidden), lambda e: (0, e))
    return pl.pallas_call(
        serve_body,
        grid=(per,),
        in_specs=[pl.BlockSpec((arrays, parts, groups, 1, rows, hidden), lambda e: (0, 0, 0, e, 0, 0))],
        out_specs=[block, block, block],
        out_shape=[out, out, out],
        compiler_params=pltpu.CompilerParams(vmem_limit_bytes=60 * 1024 * 1024),
        name="serve",
    )(staged)


def direct_shards(
    prompt, norm_gain, gate_master, up_master, down_master, group_choice, inner_choice, route_weight
):
    groups, parts = lax.axis_size("fs"), lax.axis_size("tp")
    cast = cast_masters(norm_gain, gate_master, up_master, down_master, groups)
    staged, mixed = spread(cast, prompt, group_choice, inner_choice, route_weight, parts)
    gate_local, up_local, down_local = serve(staged)
    return (gate_local, up_local, down_local, mixed)


def fits_direct(mesh):
    groups, parts = mesh.shape["fs"], mesh.shape["tp"]
    whole_experts = (GROUPS * EPG) % groups == 0 and (GROUPS * EPG // groups) % 2 == 0
    return parts == 4 and groups >= 4 and groups & (groups - 1) == 0 and whole_experts and FF // parts % 128 == 0


def solution(mesh):
    in_specs = (
        P("tp", None),
        P("fs"),
        P(None, "fs", "tp"),
        P(None, "fs", "tp"),
        P(None, "fs", "tp"),
        P("tp"),
        P("tp", None),
        P("tp", None),
    )
    out_specs = (P(None, "fs"), P(None, "fs"), P(None, "fs"), P("tp", "fs"))
    body = direct_shards if fits_direct(mesh) else shards
    return jax.shard_map(body, mesh=mesh, in_specs=in_specs, out_specs=out_specs, check_vma=False)
```
